512 devices in a mesh: kv: 64 (over z, y), tp: 8 (over x, core).
Axes of the slice: x: 4, y: 4, z: 16, core: 2. Of those that a mesh axis runs over, the one named last changes fastest.
Arguments:
- tokens: bfloat16 [256, 4096], P(None, 'kv'), may hold values from -12 to 12
- mix_gain: float32 [4096], P('kv'), may hold values from 0.1 to 1.9
- w_query: bfloat16 [4096, 2048], P('kv', 'tp'), may hold values from -0.09375 to 0.09375
- w_key: bfloat16 [4096, 2048], P('kv', 'tp'), may hold values from -0.09375 to 0.09375
- w_value: bfloat16 [4096, 2048], P('kv', 'tp'), may hold values from -0.09375 to 0.09375
- w_gate: bfloat16 [4096, 2048], P('kv', 'tp'), may hold values from -0.09375 to 0.09375
- w_beta: bfloat16 [4096, 16], P('kv', 'tp'), may hold values from -0.09375 to 0.09375
- w_decay: bfloat16 [4096, 16], P('kv', 'tp'), may hold values from -0.09375 to 0.09375
- decay_rate: float32 [16], P('tp'), may hold values from 0.05 to 3
- head_gain: float32 [128], replicated, may hold values from 0.1 to 1.9
- state: float32 [256, 16, 128, 128], P('kv', 'tp'), may hold values from -1.2 to 1.2
- w_out: bfloat16 [2048, 4096], P('tp', 'kv'), may hold values from -0.25 to 0.25
- mlp_gain: float32 [4096], P('kv'), may hold values from 0.1 to 1.9
- w_up: bfloat16 [4096, 16384], P('kv', 'tp'), may hold values from -0.09375 to 0.09375
- w_down: bfloat16 [16384, 4096], P('tp', 'kv'), may hold values from -0.046875 to 0.046875
Outputs:
- layer_out: bfloat16 [256, 4096], P(None, 'kv')
- new_state: float32 [256, 16, 128, 128], P('kv', 'tp')
The draws below stay inside these ranges and needn't reach their ends.
All inputs are finite; a program needn't handle non-finite values.
Results may differ from the reference program's by a relative error of at most 0.017.
Values may be sent and summed in bfloat16 or wider, within the bound.
A program may use at most 64 MiB of HBM per device.

```python
import math
import jax
import jax.numpy as jnp
from jax import lax

D = 4096
HEADS = 16
HEAD_DIM = 128
FF = 16384
ROWS = 256
N_TP = 8


def draw_tokens(key, part):
    columns = jnp.arange(D, dtype=jnp.float32) / D
    base = jnp.clip(jax.random.normal(key, (ROWS, D), jnp.float32), -6.0, 6.0)
    values = base * (0.5 * 4.0 ** columns)
    return values.astype(jnp.bfloat16)


def steps_of(own_key, shape, cuts, smallest, high):
    gain, own = 1.0, jax.random.fold_in(own_key, 6)
    for position, parts in cuts:
        draws = jnp.exp(jax.random.uniform(jax.random.fold_in(own, position), (parts,), jnp.float32, smallest / len(cuts), high / len(cuts)))
        gain = gain * jnp.repeat(draws, shape[position] // parts).reshape([-1 if axis == position else 1 for axis in range(len(shape))])
    return gain


def noise(key, extent, scale, limit, cuts=(), held_as=jnp.bfloat16):
    gain = steps_of(key, extent, cuts, -0.22, 0.18) if cuts else 1.0
    drawn = jax.random.normal(key, extent, jnp.float32) * scale * gain
    return jnp.minimum(jnp.maximum(drawn, -limit), limit).astype(held_as)


def setup_inputs(seed: int = 0) -> dict:
    splits = jax.random.split(jax.random.key(seed), 16)
    return {
        "tokens": draw_tokens(jax.random.fold_in(splits[15], 71), 0),
        "mix_gain": jnp.clip(1.0 + 0.18 * jax.random.normal(splits[1], (D,), jnp.float32), 0.1, 1.9),
        "w_query": noise(splits[2], (D, HEADS * HEAD_DIM), D ** -0.5, 0.09375, ((0, 64), (1, 8))),
        "w_key": noise(splits[3], (D, HEADS * HEAD_DIM), D ** -0.5, 0.09375, ((0, 64), (1, 8))),
        "w_value": noise(splits[4], (D, HEADS * HEAD_DIM), D ** -0.5, 0.09375, ((0, 64), (1, 8))),
        "w_gate": noise(splits[5], (D, HEADS * HEAD_DIM), D ** -0.5, 0.09375, ((0, 64), (1, 8))),
        "w_beta": noise(splits[6], (D, HEADS), D ** -0.5, 0.09375, ((0, 64), (1, 8))),
        "w_decay": noise(splits[7], (D, HEADS), D ** -0.5, 0.09375, ((0, 64), (1, 8))),
        "decay_rate": jnp.clip(jnp.exp(math.log(3.0) - 4.0943445 * jax.random.uniform(splits[8], (HEADS,), jnp.float32) ** steps_of(splits[8], (HEADS,), ((0, 8),), -0.2, 0.2)), 0.05, 3.0),
        "head_gain": jnp.clip(1.0 + 0.18 * jax.random.normal(splits[9], (HEAD_DIM,), jnp.float32), 0.1, 1.9),
        "state": noise(splits[10], (ROWS, HEADS, HEAD_DIM, HEAD_DIM), 0.2, 1.2, ((0, 64), (1, 8)), jnp.float32),
        "w_out": noise(splits[11], (HEADS * HEAD_DIM, D), (HEADS * HEAD_DIM // 4) ** -0.5, 0.25, ((0, 8), (1, 64))),
        "mlp_gain": jnp.clip(1.0 + 0.18 * jax.random.normal(splits[12], (D,), jnp.float32), 0.1, 1.9),
        "w_up": noise(splits[13], (D, FF), D ** -0.5, 0.09375, ((0, 64), (1, 8))),
        "w_down": noise(splits[14], (FF, D), FF ** -0.5, 0.046875, ((0, 8), (1, 64))),
    }


norm_eps = 1e-06

def rms_scale(values):
    return lax.rsqrt(lax.optimization_barrier(jnp.mean(values * values, axis=-1, keepdims=True)) + norm_eps)

def delta_update(query_pre, key_pre, value_pre, gate_pre, beta_pre, decay_pre, decay_rate, head_gain, state):
    f32 = jnp.float32
    query = jax.nn.silu(query_pre)
    query = query * lax.rsqrt(lax.optimization_barrier(jnp.sum(query * query, axis=-1, keepdims=True)) + norm_eps) * query.shape[-1] ** (-0.5)
    keyed = jax.nn.silu(key_pre)
    keyed = keyed * lax.rsqrt(lax.optimization_barrier(jnp.sum(keyed * keyed, axis=-1, keepdims=True)) + norm_eps)
    valued = jax.nn.silu(value_pre)
    beta = jax.nn.sigmoid(beta_pre)
    decay = jnp.exp(-decay_rate.astype(f32) * jax.nn.softplus(decay_pre))
    recalled = jnp.einsum('bhk,bhkv->bhv', keyed, state, precision=lax.Precision.HIGHEST)
    corrected = state - beta[:, :, None, None] * keyed[:, :, :, None] * recalled[:, :, None, :]
    new_state = decay[:, :, None, None] * corrected + beta[:, :, None, None] * keyed[:, :, :, None] * valued[:, :, None, :]
    read = jnp.einsum('bhkv,bhk->bhv', new_state, query, precision=lax.Precision.HIGHEST)
    mixed = read * rms_scale(read) * head_gain.astype(f32) * jax.nn.silu(gate_pre)
    return (mixed, new_state)

def reference(tokens, mix_gain, w_query, w_key, w_value, w_gate, w_beta, w_decay, decay_rate, head_gain, state, w_out, mlp_gain, w_up, w_down):
    f32 = jnp.float32
    bf16 = jnp.bfloat16
    rows = tokens.shape[0]
    tok32 = tokens.astype(f32)
    scale = rms_scale(tok32)
    gained = (tok32 * mix_gain.astype(f32)).astype(bf16)

    def project(weight):
        return jnp.dot(gained, weight, preferred_element_type=f32) * scale

    def heads_view(values):
        return values.reshape(rows, HEADS, HEAD_DIM)
    mixed, new_state = delta_update(heads_view(project(w_query)), heads_view(project(w_key)), heads_view(project(w_value)), heads_view(project(w_gate)), project(w_beta), project(w_decay), decay_rate, head_gain, state)
    mixed = mixed.reshape(rows, HEADS * HEAD_DIM).astype(bf16)
    group = HEADS * HEAD_DIM // N_TP
    attended = jnp.zeros((rows, D), f32)
    for index in range(N_TP):
        term = jnp.dot(mixed[:, index * group:(index + 1) * group], w_out[index * group:(index + 1) * group], preferred_element_type=f32)
        attended = attended + lax.optimization_barrier(term.astype(bf16)).astype(f32)
    residual = lax.optimization_barrier((tok32 + attended).astype(bf16)).astype(f32)
    scale_mid = rms_scale(residual)
    gained_mid = (residual * mlp_gain.astype(f32)).astype(bf16)
    up_pre = jnp.dot(gained_mid, w_up, preferred_element_type=f32) * scale_mid
    hidden = jnp.square(jax.nn.relu(up_pre)).astype(bf16)
    width = FF // N_TP
    mixer = jnp.zeros((rows, D), f32)
    for index in range(N_TP):
        term = jnp.dot(hidden[:, index * width:(index + 1) * width], w_down[index * width:(index + 1) * width], preferred_element_type=f32)
        mixer = mixer + lax.optimization_barrier(term.astype(bf16)).astype(f32)
    layer_out = (residual + mixer).astype(bf16)
    return (layer_out, new_state)
```

```python
import functools

import jax
import jax.numpy as jnp
from jax import lax
from jax.experimental import pallas as pl
from jax.experimental.pallas import tpu as pltpu
from jax.sharding import PartitionSpec as P

D = 4096
EPS = 1e-06
MESH = pl.DeviceIdType.MESH
F32 = jnp.float32
BF16 = jnp.bfloat16
NZ, NY, NT = 16, 4, 8
FAR_FIRST = (8, 7, 9, 6, 10, 5, 11, 4, 12, 3, 13, 2, 14, 1, 15)

NN = (((1,), (0,)), ((), ()))
NT_DIMS = (((1,), (1,)), ((), ()))


def mm(a, b, dims=NN):
    return lax.dot_general(a, b, dims, preferred_element_type=F32)


def iota(shape, dim):
    return lax.broadcasted_iota(jnp.int32, shape, dim)


def one_hot(cond):
    return jnp.where(cond, 1.0, 0.0).astype(BF16)


class Wire:
    def __init__(self, send_sem, recv_sem):
        self.send_sem, self.recv_sem = send_sem, recv_sem
        self.count, self.sent = 0, []

    def send(self, src, dst, landed, kv, tp):
        k = self.count
        self.count += 1
        copy = pltpu.make_async_remote_copy(
            src, dst, self.send_sem.at[k], self.recv_sem.at[k],
            device_id={"kv": kv, "tp": tp}, device_id_type=MESH,
        )
        copy.start()
        self.sent.append(copy)
        return pltpu.make_async_remote_copy(
            src, landed, self.send_sem.at[k], self.recv_sem.at[k],
            device_id={"kv": kv, "tp": tp}, device_id_type=MESH,
        )

    def finish(self):
        for copy in self.sent:
            copy.wait_send()


def kernel(
    tok_ref, mixg_ref, wq_ref, wk_ref, wv_ref, wg_ref, small_ref, rate_ref, hgain_ref,
    state_ref, wo_ref, mlpg_ref, wu_ref, wd_ref,
    out_ref, new_ref,
    wqf, wkf, wvf, wgf, wof, wuf, wdf, st, stn,
    tg_s, tg, sm, mg, sa, sb, ra, rb, mx, at, ru_s, ru, hid, res_s, res, fin_s, fin, rd,
    onehots, send_sem, recv_sem, local_sem,
):
    kv, tp = lax.axis_index("kv"), lax.axis_index("tp")
    z, y = kv // NY, kv % NY

    def kv_of(zz, yy):
        return zz * NY + yy

    def zp(d):
        return (z + d) % NZ

    def yp(d):
        return (y + d) % NY

    def tq(d):
        return (tp + d) % NT

    barrier = pltpu.get_barrier_semaphore()
    for d in range(1, NZ):
        pl.semaphore_signal(barrier, 1, device_id={"kv": kv_of(zp(d), y), "tp": tp}, device_id_type=MESH)
    for d in range(1, NY):
        pl.semaphore_signal(barrier, 1, device_id={"kv": kv_of(z, yp(d)), "tp": tp}, device_id_type=MESH)
    for e in range(NY):
        for d in range(1, NT):
            pl.semaphore_signal(barrier, 1, device_id={"kv": kv_of(z, yp(e)), "tp": tq(d)}, device_id_type=MESH)

    loads = []
    for i, (src, dst) in enumerate((
        (wq_ref, wqf.at[y]), (wk_ref, wkf.at[y]), (wv_ref, wvf.at[y]), (wg_ref, wgf.at[y]),
        (wo_ref, wof.at[y]), (wu_ref, wuf.at[y]), (wd_ref, wdf.at[y]), (state_ref, st),
    )):
        load = pltpu.make_async_copy(src, dst, local_sem.at[i])
        load.start()
        loads.append(load)

    r64, c64 = iota((64, 64), 0), iota((64, 64), 1)
    eye64 = one_hot(r64 == c64)
    gain_col = jnp.sum(jnp.where(r64 == c64, jnp.broadcast_to(mixg_ref[...], (64, 64)), 0.0), axis=1, keepdims=True)
    tokt = tok_ref[...]
    gnt = (tokt.astype(F32) * gain_col).astype(BF16)
    rr, cc = iota((256, 128), 0), iota((256, 128), 1)
    cl = cc % 64
    for yy in range(NY):
        row_of = 16 * (cl // 4) + 4 * yy + cl % 4
        hit = rr == row_of
        pick_t = one_hot(hit & (cc < 64))
        pick_g = one_hot(hit & (cc >= 64))
        tg_s[yy] = (mm(tokt, pick_t) + mm(gnt, pick_g)).astype(BF16)
    lane = iota((8, 256), 1)
    mg[pl.ds(y, 1)] = jnp.where(lane // 64 == y, jnp.broadcast_to(mlpg_ref[...], (8, 256)), 0.0)[None]
    sm[pl.ds(y, 1)] = small_ref[...][None]
    tg[pl.ds(y, 1)] = tg_s[pl.ds(y, 1)]

    rr, cc = iota((128, 128), 0), iota((128, 128), 1)
    src_row = 4 * (rr // 8) + rr % 4
    half = (rr % 8) // 4
    q_g = [one_hot((cc == 64 + src_row) & (half == h)) for h in range(2)]
    q_t = one_hot(cc == src_row)
    rr2, cc2 = iota((64, 128), 0), iota((64, 128), 1)
    pick_tok = one_hot(cc2 == rr2)
    for h in range(2):
        onehots[h] = one_hot(cc2 == 8 * (rr2 // 4) + 4 * h + rr2 % 4)

    wire = Wire(send_sem, recv_sem)
    pl.semaphore_wait(barrier, (NZ - 1) + (NY - 1) + NY * (NT - 1))

    def y_send(buf, d):
        return wire.send(buf.at[y], buf.at[y], buf.at[yp(-d)], kv_of(z, yp(d)), tp)

    got = []
    for d in (1, 3, 2):
        got.append(wire.send(tg_s.at[yp(d)], tg.at[y], tg.at[yp(-d)], kv_of(z, yp(d)), tp))
        got.append(y_send(sm, d))
        got.append(y_send(mg, d))
    for i in range(4):
        loads[i].wait()
    full = (wqf, wkf, wvf, wgf)
    right, left = [None] * 4, [None] * 4
    relay = [None] * 4
    for pair in ((0, 1), (2, 3)):
        for i in pair:
            right[i] = y_send(full[i], 1)
            left[i] = y_send(full[i], 3)
        a, b = pair
        right[a].wait_recv()
        relay[a] = wire.send(full[a].at[yp(-1)], full[a].at[yp(-1)], full[a].at[yp(-2)], kv_of(z, yp(1)), tp)
        left[b].wait_recv()
        relay[b] = wire.send(full[b].at[yp(1)], full[b].at[yp(1)], full[b].at[yp(2)], kv_of(z, yp(-1)), tp)
    loads[4].wait()
    loads[5].wait()
    loads[6].wait()
    wo_got = [y_send(wof, d) for d in (1, 3, 2)]
    wu_got = [y_send(wuf, d) for d in (1, 3)]

    for g in got:
        g.wait_recv()
    tgv = tg[...].reshape(256, 128)
    lq = [mm(q_g[h], tgv, NT_DIMS).astype(BF16) for h in range(2)]
    tok_rows = mm(pick_tok, tgv, NT_DIMS)

    t32 = tgv.astype(F32)
    energy = jnp.sum(t32 * t32, axis=0, keepdims=True)
    e_hi = energy.astype(BF16)
    e_lo = (energy - e_hi.astype(F32)).astype(BF16)
    e_rows = jnp.where(rr == 2, jnp.broadcast_to(e_hi.astype(F32), (128, 128)),
                       jnp.where(rr == 3, jnp.broadcast_to(e_lo.astype(F32), (128, 128)), 0.0)).astype(BF16)
    small_out = mm(q_t, e_rows, NT_DIMS)
    for h in range(2):
        sel = one_hot(((iota((128, 8), 0) == 0) & (iota((128, 8), 1) == h))
                      | ((iota((128, 8), 0) == 1) & (iota((128, 8), 1) == 2 + h)))
        parts = [mm(eye64, mm(sel, sm[yy][:, :64]).astype(BF16), NT_DIMS) for yy in range(NY)]
        w_small = jnp.concatenate(parts, axis=0).astype(BF16)
        small_out += mm(lq[h], w_small)

    def project(buf):
        w = buf[...].reshape(256, 256)
        return mm(lq[0], w[:, :128]) + mm(lq[1], w[:, 128:])

    def stage(blocks):
        return jnp.concatenate([b.reshape(NZ, 8, 128) for b in blocks], axis=1).astype(BF16)

    def z_scatter(src, dst):
        return [wire.send(src.at[zp(d)], dst.at[z], dst.at[zp(-d)], kv_of(zp(d), y), tp) for d in FAR_FIRST]

    for i, which in ((0, relay), (1, relay)):
        which[i].wait_recv()
    left[0].wait_recv()
    right[1].wait_recv()
    staged = stage([project(wqf), project(wkf), small_out])
    sa[...] = staged
    got_a = z_scatter(sa, ra)
    relay[2].wait_recv()
    relay[3].wait_recv()
    left[2].wait_recv()
    right[3].wait_recv()
    sb[...] = stage([project(wvf), project(wgf)])
    got_b = z_scatter(sb, rb)
    ra[pl.ds(z, 1)] = sa[pl.ds(z, 1)]
    rb[pl.ds(z, 1)] = sb[pl.ds(z, 1)]
    loads[7].wait()
    for g in got_a:
        g.wait_recv()
    sum_a = jnp.sum(ra[...].astype(F32), axis=0)
    extra = sum_a[16:24]
    scale = lax.rsqrt((extra[:, 2:3] + extra[:, 3:4]) * (1.0 / D) + EPS)
    query = jax.nn.silu(sum_a[0:8] * scale)
    query = query * lax.rsqrt(jnp.sum(query * query, axis=1, keepdims=True) + EPS) * (128 ** -0.5)
    keyed = jax.nn.silu(sum_a[8:16] * scale)
    keyed = keyed * lax.rsqrt(jnp.sum(keyed * keyed, axis=1, keepdims=True) + EPS)
    beta = jax.nn.sigmoid(extra[:, 0:1] * scale)
    decay = jnp.exp(-rate_ref[:, 0:1] * jax.nn.softplus(extra[:, 1:2] * scale))
    key_t = jnp.transpose(keyed)
    query_t = jnp.transpose(query)
    recs = []
    for b in range(8):
        h, i = b // 4, b % 4
        recs.append(jnp.sum(st[i, h] * key_t[:, b:b + 1], axis=0, keepdims=True))
    recalled = jnp.concatenate(recs, axis=0)
    for g in got_b:
        g.wait_recv()
    sum_b = jnp.sum(rb[...].astype(F32), axis=0)
    valued = jax.nn.silu(sum_b[0:8] * scale)
    gate = jax.nn.silu(sum_b[8:16] * scale)
    write = beta * (valued - decay * recalled)
    reads = []
    for b in range(8):
        h, i = b // 4, b % 4
        fresh = decay[b:b + 1, :] * st[i, h] + key_t[:, b:b + 1] * write[b:b + 1, :]
        stn[i, h] = fresh
        reads.append(jnp.sum(fresh * query_t[:, b:b + 1], axis=0, keepdims=True))
    read = jnp.concatenate(reads, axis=0)
    mixed = read * lax.rsqrt(jnp.mean(read * read, axis=1, keepdims=True) + EPS) * hgain_ref[...] * gate
    mx[pl.ds(z, 1)] = mixed.astype(BF16)[None]

    def z_gather(buf):
        return [wire.send(buf.at[z], buf.at[z], buf.at[zp(-d)], kv_of(zp(d), y), tp) for d in FAR_FIRST]

    got_m = z_gather(mx)
    store = pltpu.make_async_copy(stn, new_ref, local_sem.at[8])
    store.start()
    wu_got[0].wait_recv()
    wu_got[1].wait_recv()
    wu_far = [
        wire.send(wuf.at[yp(-1), pl.ds(0, 32)], wuf.at[yp(-1), pl.ds(0, 32)], wuf.at[yp(-2), pl.ds(0, 32)], kv_of(z, yp(1)), tp),
        wire.send(wuf.at[yp(1), pl.ds(32, 32)], wuf.at[yp(1), pl.ds(32, 32)], wuf.at[yp(2), pl.ds(32, 32)], kv_of(z, yp(-1)), tp),
    ]
    wd_got = [y_send(wdf, d) for d in (1, 3)]
    for g in wo_got:
        g.wait_recv()
    for g in got_m:
        g.wait_recv()
    m = mx[...].astype(F32).reshape(128, 128).astype(BF16)
    mixed2 = jnp.concatenate([mm(onehots[h], m) for h in range(2)], axis=1).astype(BF16)
    at[pl.ds(tp, 1)] = mm(mixed2, wof[...].reshape(256, 256), NT_DIMS).astype(BF16)[None]
    got_t = [wire.send(at.at[tp], at.at[tp], at.at[tq(-d)], kv, tq(d)) for d in (4, 5, 2, 3, 6, 7, 1)]
    gain_mid = jnp.sum(mg[...], axis=0)[0:1]
    for g in got_t:
        g.wait_recv()
    attended = jnp.sum(at[...].astype(F32), axis=0)
    residual = (tok_rows + attended).astype(BF16)
    r32 = residual.astype(F32)
    gained_mid = (r32 * gain_mid).astype(BF16)
    rr3, cc3 = iota((128, 64), 0), iota((128, 64), 1)
    row3 = 4 * (rr3 // 8) + rr3 % 4
    half3 = (rr3 % 8) // 4
    em = jnp.sum(r32 * r32, axis=1, keepdims=True)
    em_hi = em.astype(BF16).astype(F32)
    em_lo = em - em_hi
    lane3 = iota((64, 128), 1)
    em_mat = jnp.where(lane3 == 0, em_hi, jnp.where(lane3 == 1, em_lo, 0.0)).astype(BF16)
    ru_s[:, :, 1024:] = mm(one_hot(cc3 == row3), em_mat).reshape(NZ, 8, 128).astype(BF16)
    lg = [mm(one_hot((cc3 == row3) & (half3 == c)), gained_mid).astype(BF16) for c in range(2)]
    for g in wu_far:
        g.wait_recv()
    wu = wuf[...].reshape(256, 2048)
    up = mm(lg[0], wu[:, :1024]) + mm(lg[1], wu[:, 1024:])
    ru_s[:, :, :1024] = up.reshape(NZ, 8, 1024).astype(BF16)
    got_u = z_scatter(ru_s, ru)
    ru[pl.ds(z, 1)] = ru_s[pl.ds(z, 1)]

    eye256 = one_hot(iota((256, 256), 0) == iota((256, 256), 1))

    def by_y(x):
        x = x.reshape(NY, 2, 32, 64)
        return jnp.concatenate([x[:, 0], x[:, 1]], axis=-1).astype(BF16)

    res_s[...] = by_y(mm(eye256, residual, NT_DIMS))
    res[pl.ds(y, 1)] = res_s[pl.ds(y, 1)]
    got_r = [wire.send(res_s.at[yp(d)], res.at[y], res.at[yp(-d)], kv_of(z, yp(d)), tp) for d in (1, 3, 2)]
    wd_got[0].wait_recv()
    wd_got[1].wait_recv()
    wd_far = [
        wire.send(wdf.at[yp(-1), pl.ds(0, 32)], wdf.at[yp(-1), pl.ds(0, 32)], wdf.at[yp(-2), pl.ds(0, 32)], kv_of(z, yp(1)), tp),
        wire.send(wdf.at[yp(1), pl.ds(32, 32)], wdf.at[yp(1), pl.ds(32, 32)], wdf.at[yp(2), pl.ds(32, 32)], kv_of(z, yp(-1)), tp),
    ]
    for g in got_u:
        g.wait_recv()
    total = jnp.sum(ru[...].astype(F32), axis=0)
    scale_mid = lax.rsqrt((total[:, 1024:1025] + total[:, 1025:1026]) * (1.0 / D) + EPS)
    hidden = jnp.square(jnp.maximum(total[:, :1024] * scale_mid, 0.0))
    hid[pl.ds(z, 1)] = hidden.astype(BF16)[None]
    got_h = z_gather(hid)
    for g in wd_far:
        g.wait_recv()
    for g in got_r:
        g.wait_recv()
    for g in got_h:
        g.wait_recv()
    hv = hid[...].astype(F32).reshape(128, 1024).astype(BF16)
    wd = wdf[...].reshape(256, 2048)
    down = None
    for c in range(2):
        rows = mm(onehots[c], hv).astype(BF16)
        term = mm(wd[:, 1024 * c:1024 * (c + 1)], rows, NT_DIMS)
        down = term if down is None else down + term
    fin_s[...] = by_y(down)
    got_f = []
    for e in (2, 1, 3, 0):
        for d in (4, 5, 2, 3, 6, 7, 1, 0):
            if e == 0 and d == 0:
                continue
            got_f.append(wire.send(
                fin_s.at[yp(e)], fin.at[tp, y], fin.at[tq(-d), yp(-e)], kv_of(z, yp(e)), tq(d)))
    fin[pl.ds(tp, 1), pl.ds(y, 1)] = fin_s[pl.ds(y, 1)][None]
    for g in got_f:
        g.wait_recv()
    mixer = jnp.sum(fin[...].astype(F32), axis=0)
    last = (res[...].astype(F32) + mixer).astype(BF16)
    flat = jnp.concatenate([last[yy] for yy in range(NY)], axis=1)
    rr4, cc4 = iota((512, 256), 0), iota((512, 256), 1)
    row4 = 16 * ((rr4 % 64) // 4) + 4 * (rr4 // 128) + rr4 % 4
    for e in range(2):
        place = one_hot((cc4 == row4) & ((rr4 % 128) // 64 == e))
        out_ref[pl.ds(32 * e, 32), :] = mm(flat, place).astype(BF16)
    store.wait()
    wire.finish()


def body(
    tokens, mix_gain, w_query, w_key, w_value, w_gate, w_beta, w_decay, decay_rate, head_gain,
    state, w_out, mlp_gain, w_up, w_down,
):
    small = jnp.concatenate([w_beta.T, w_decay.T, jnp.zeros((4, 64), BF16)], axis=0)
    small = jnp.pad(small, ((0, 0), (0, 64)))
    rate = jnp.broadcast_to(jnp.repeat(decay_rate, 4)[:, None], (8, 128))
    gain4 = jnp.concatenate([mlp_gain] * 4).reshape(1, 256)
    vmem = pl.BlockSpec(memory_space=pltpu.VMEM)
    hbm = pl.BlockSpec(memory_space=pltpu.HBM)
    v = pltpu.VMEM
    n_sem = 160
    out, new = pl.pallas_call(
        kernel,
        name="layer",
        out_shape=(
            jax.ShapeDtypeStruct((64, 256), BF16),
            jax.ShapeDtypeStruct((4, 2, 128, 128), F32),
        ),
        in_specs=[vmem, vmem, hbm, hbm, hbm, hbm, vmem, vmem, vmem, hbm, hbm, vmem, hbm, hbm],
        out_specs=(vmem, hbm),
        scratch_shapes=[
            v((4, 64, 256), BF16), v((4, 64, 256), BF16), v((4, 64, 256), BF16), v((4, 64, 256), BF16),
            v((4, 64, 256), BF16), v((4, 64, 2048), BF16), v((4, 64, 2048), BF16),
            v((4, 2, 128, 128), F32), v((4, 2, 128, 128), F32),
            v((4, 64, 128), BF16), v((4, 64, 128), BF16), v((4, 8, 128), BF16), v((4, 8, 256), F32),
            v((16, 24, 128), BF16), v((16, 16, 128), BF16), v((16, 24, 128), BF16), v((16, 16, 128), BF16),
            v((16, 8, 128), BF16), v((8, 64, 256), BF16),
            v((16, 8, 1152), BF16), v((16, 8, 1152), BF16), v((16, 8, 1024), BF16),
            v((4, 32, 128), BF16), v((4, 32, 128), BF16),
            v((4, 32, 128), BF16), v((8, 4, 32, 128), BF16), v((8, 128), F32),
            v((2, 64, 128), BF16),
            pltpu.SemaphoreType.DMA((n_sem,)), pltpu.SemaphoreType.DMA((n_sem,)),
            pltpu.SemaphoreType.DMA((9,)),
        ],
        compiler_params=pltpu.CompilerParams(
            collective_id=0, has_side_effects=True, vmem_limit_bytes=48 * 1024 * 1024,
        ),
    )(
        tokens.T, mix_gain.reshape(1, 64), w_query, w_key, w_value, w_gate, small, rate,
        head_gain.reshape(1, 128), state, w_out.T, gain4, w_up, w_down.T,
    )
    return out.T, new


def solution(mesh):
    return jax.shard_map(
        body,
        mesh=mesh,
        in_specs=(
            P(None, "kv"), P("kv"), P("kv", "tp"), P("kv", "tp"), P("kv", "tp"), P("kv", "tp"),
            P("kv", "tp"), P("kv", "tp"), P("tp"), P(), P("kv", "tp", None, None),
            P("tp", "kv"), P("kv"), P("kv", "tp"), P("tp", "kv"),
        ),
        out_specs=(P(None, "kv"), P("kv", "tp", None, None)),
        check_vma=False,
    )
```

```python
import functools

import jax
import jax.numpy as jnp
from jax import lax
from jax.experimental import pallas as pl
from jax.experimental.pallas import tpu as pltpu
from jax.sharding import PartitionSpec as P

D = 4096
EPS = 1e-06
MESH = pl.DeviceIdType.MESH
F32 = jnp.float32
BF16 = jnp.bfloat16
NZ, NY, NT = 16, 4, 8
FAR_FIRST = (8, 7, 9, 6, 10, 5, 11, 4, 12, 3, 13, 2, 14, 1, 15)

NN = (((1,), (0,)), ((), ()))
NT_DIMS = (((1,), (1,)), ((), ()))


def mm(a, b, dims=NN):
    return lax.dot_general(a, b, dims, preferred_element_type=F32)


def iota(shape, dim):
    return lax.broadcasted_iota(jnp.int32, shape, dim)


def one_hot(cond):
    return jnp.where(cond, 1.0, 0.0).astype(BF16)


class Group:
    def __init__(self, wire, index, name):
        self.wire, self.index, self.name, self.total = wire, index, name, None

    def copy(self, src, dst, kv, tp):
        return pltpu.make_async_remote_copy(
            src, dst, self.wire.send_sem.at[self.index], self.wire.recv_sem.at[self.index],
            device_id={"kv": kv, "tp": tp}, device_id_type=MESH,
        )

    def send(self, src, dst, kv, tp):
        self.copy(src, dst, kv, tp).start()

    def take(self, total):
        self.total = total
        with jax.named_scope(self.name):
            self.copy(total, total, self.wire.kv, self.wire.tp).wait_recv()

    def finish(self):
        self.copy(self.total, self.total, self.wire.kv, self.wire.tp).wait_send()


class Wire:
    def __init__(self, send_sem, recv_sem, kv, tp):
        self.send_sem, self.recv_sem, self.kv, self.tp = send_sem, recv_sem, kv, tp
        self.groups = []

    def group(self, name):
        self.groups.append(Group(self, len(self.groups), name))
        return self.groups[-1]

    def finish(self):
        for group in self.groups:
            group.finish()


def kernel(
    tok_ref, mixg_ref, wq_ref, wk_ref, wv_ref, wg_ref, wb_ref, wdec_ref, rate_ref, hgain_ref,
    state_ref, wo_ref, mlpg_ref, wu_ref, wd_ref,
    out_ref, new_ref,
    tokv, mixv, wbv, wdecv, ratev, hgainv, mlpv,
    wqf, wkf, wvf, wgf, wof, wuf, wdf, st,
    tg_s, tg, sm, mg, sa, sb, ra, rb, mx, at, us, near, fs, ru, hid, em, res_s, res, fin_s, fin,
    heads_in, hid_in, place, send_sem, recv_sem, local_sem,
):
    kv, tp = lax.axis_index("kv"), lax.axis_index("tp")
    z, y = kv // NY, kv % NY

    def kv_of(zz, yy):
        return zz * NY + yy

    def zp(d):
        return (z + d) % NZ

    def yp(d):
        return (y + d) % NY

    def tq(d):
        return (tp + d) % NT

    barrier = pltpu.get_barrier_semaphore()
    for d in range(1, NZ):
        pl.semaphore_signal(barrier, 1, device_id={"kv": kv_of(zp(d), y), "tp": tp}, device_id_type=MESH)
    for d in range(1, NY):
        pl.semaphore_signal(barrier, 1, device_id={"kv": kv_of(z, yp(d)), "tp": tp}, device_id_type=MESH)
    for e in range(NY):
        for d in range(1, NT):
            pl.semaphore_signal(barrier, 1, device_id={"kv": kv_of(z, yp(e)), "tp": tq(d)}, device_id_type=MESH)

    loads = []
    for i, (src, dst) in enumerate((
        (tok_ref, tokv), (mixg_ref, mixv), (wb_ref, wbv), (wdec_ref, wdecv), (mlpg_ref, mlpv),
        (rate_ref, ratev), (hgain_ref, hgainv),
        (wq_ref, wqf.at[y]), (wk_ref, wkf.at[y]), (wv_ref, wvf.at[y]), (wg_ref, wgf.at[y]),
        (wo_ref, wof.at[y]), (wu_ref, wuf.at[y]), (wd_ref, wdf.at[y]), (state_ref, st),
    )):
        load = pltpu.make_async_copy(src, dst, local_sem.at[i])
        load.start()
        loads.append(load)

    with jax.named_scope("small_loads"):
        for i in range(7):
            loads[i].wait()

    r64, c64 = iota((64, 64), 0), iota((64, 64), 1)
    eye64 = one_hot(r64 == c64)
    gain_col = jnp.sum(jnp.where(r64 == c64, jnp.broadcast_to(mixv[...], (64, 64)), 0.0), axis=1, keepdims=True)
    tokt = tokv[...]
    gnt = (tokt.astype(F32) * gain_col).astype(BF16)
    rr, cc = iota((256, 128), 0), iota((256, 128), 1)
    cl = cc % 64
    for yy in range(NY):
        row_of = 16 * (cl // 4) + 4 * yy + cl % 4
        hit = rr == row_of
        pick_t = one_hot(hit & (cc < 64))
        pick_g = one_hot(hit & (cc >= 64))
        tg_s[yy] = (mm(tokt, pick_t) + mm(gnt, pick_g)).astype(BF16)
    mg[pl.ds(y, 1)] = jnp.broadcast_to(mlpv[...], (8, 64))[None]
    wb32, wdec32 = wbv[...].astype(F32), wdecv[...].astype(F32)
    r8 = iota((8, 64), 0)
    sm_rows = jnp.zeros((8, 64), F32)
    for k, row in enumerate((wb32[0:1], wb32[1:2], wdec32[0:1], wdec32[1:2])):
        sm_rows = jnp.where(r8 == k, jnp.broadcast_to(row, (8, 64)), sm_rows)
    sm[pl.ds(y, 1)] = sm_rows.astype(BF16)[None]
    tg[pl.ds(y, 1)] = tg_s[pl.ds(y, 1)]

    rr, cc = iota((128, 128), 0), iota((128, 128), 1)
    src_row = 4 * (rr // 8) + rr % 4
    half = (rr % 8) // 4
    q_g = [one_hot((cc == 64 + src_row) & (half == h)) for h in range(2)]
    q_t = one_hot(cc == src_row)
    rr2, cc2 = iota((64, 128), 0), iota((64, 128), 1)
    pick_tok = one_hot(cc2 == rr2)
    z2 = rr2 // 4
    for h in range(2):
        heads_in[h] = one_hot(cc2 == 8 * z2 + 4 * h + rr2 % 4)
        hid_in[h] = one_hot(cc2 == 64 * (z2 % 2) + 8 * (z2 // 2) + 4 * h + rr2 % 4)

    wire = Wire(send_sem, recv_sem, kv, tp)
    with jax.named_scope("barrier"):
        pl.semaphore_wait(barrier, (NZ - 1) + (NY - 1) + NY * (NT - 1))

    def y_send(group, buf, d, src=None):
        group.send(buf.at[y] if src is None else src, buf.at[y], kv_of(z, yp(d)), tp)

    g_tg, g_sm, g_mg = wire.group("g_tg"), wire.group("g_sm"), wire.group("g_mg")
    for d in (1, 3, 2):
        y_send(g_tg, tg, d, tg_s.at[yp(d)])
        y_send(g_sm, sm, d)
    for i in range(4):
        loads[7 + i].wait()
    full = (wqf, wkf, wvf, wgf)
    right = [wire.group("right") for _ in range(4)]
    left = [wire.group("left") for _ in range(4)]
    relay = [wire.group("relay") for _ in range(4)]
    for i in range(4):
        y_send(right[i], full[i], 1)
        y_send(left[i], full[i], 3)

    def pass_on(a, b):
        right[a].take(full[a].at[yp(-1)])
        relay[a].send(full[a].at[yp(-1)], full[a].at[yp(-1)], kv_of(z, yp(1)), tp)
        left[b].take(full[b].at[yp(1)])
        relay[b].send(full[b].at[yp(1)], full[b].at[yp(1)], kv_of(z, yp(-1)), tp)

    g_tg.take(tg.at[pl.ds(0, 3)])
    g_sm.take(sm.at[pl.ds(0, 3)])
    pass_on(0, 1)
    tgv = tg[...].reshape(256, 128)
    lq = [mm(q_g[h], tgv, NT_DIMS).astype(BF16) for h in range(2)]
    tok_rows = mm(pick_tok, tgv, NT_DIMS)

    t32 = tgv.astype(F32)
    energy = jnp.sum(t32 * t32, axis=0, keepdims=True)
    e_hi = energy.astype(BF16)
    e_lo = (energy - e_hi.astype(F32)).astype(BF16)
    e_rows = jnp.where(rr == 2, jnp.broadcast_to(e_hi.astype(F32), (128, 128)),
                       jnp.where(rr == 3, jnp.broadcast_to(e_lo.astype(F32), (128, 128)), 0.0)).astype(BF16)
    small_out = mm(q_t, e_rows, NT_DIMS)
    for h in range(2):
        sel = one_hot(((iota((128, 8), 0) == 0) & (iota((128, 8), 1) == h))
                      | ((iota((128, 8), 0) == 1) & (iota((128, 8), 1) == 2 + h)))
        parts = [mm(eye64, mm(sel, sm[yy]).astype(BF16), NT_DIMS) for yy in range(NY)]
        w_small = jnp.concatenate(parts, axis=0).astype(BF16)
        small_out += mm(lq[h], w_small)
    pass_on(2, 3)
    for i in range(11, 14):
        loads[i].wait()
    g_wo, g_wu, g_wu2 = wire.group("g_wo"), wire.group("g_wu"), wire.group("g_wu2")
    g_wd, g_wd2 = wire.group("g_wd"), wire.group("g_wd2")
    for d in (1, 3, 2):
        y_send(g_wo, wof, d)
    for d in (1, 3, 2):
        y_send(g_mg, mg, d)
    for d in (1, 3):
        y_send(g_wu, wuf, d)

    def project(buf):
        w = buf[...].reshape(256, 256)
        return mm(lq[0], w[:, :128]) + mm(lq[1], w[:, 128:])

    def stage(blocks):
        return jnp.concatenate([b.reshape(NZ, 8, 128) for b in blocks], axis=1).astype(BF16)

    def z_scatter(group, src, dst):
        for d in FAR_FIRST:
            group.send(src.at[zp(d)], dst.at[z], kv_of(zp(d), y), tp)

    def z_gather(group, buf):
        for d in FAR_FIRST:
            group.send(buf.at[z], buf.at[z], kv_of(zp(d), y), tp)

    def z_take(group, buf):
        group.take(buf.at[pl.ds(0, NZ - 1)])

    g_a, g_b, g_m = wire.group("g_a"), wire.group("g_b"), wire.group("g_m")
    left[0].take(wqf.at[yp(1)])
    relay[0].take(wqf.at[yp(2)])
    right[1].take(wkf.at[yp(-1)])
    relay[1].take(wkf.at[yp(2)])
    sa[...] = stage([project(wqf), project(wkf), small_out])
    z_scatter(g_a, sa, ra)
    left[2].take(wvf.at[yp(1)])
    relay[2].take(wvf.at[yp(2)])
    right[3].take(wgf.at[yp(-1)])
    relay[3].take(wgf.at[yp(2)])
    sb[...] = stage([project(wvf), project(wgf)])
    z_scatter(g_b, sb, rb)
    ra[pl.ds(z, 1)] = sa[pl.ds(z, 1)]
    rb[pl.ds(z, 1)] = sb[pl.ds(z, 1)]
    loads[14].wait()
    z_take(g_a, ra)
    sum_a = jnp.sum(ra[...].astype(F32), axis=0)
    extra = sum_a[16:24]
    scale = lax.rsqrt((extra[:, 2:3] + extra[:, 3:4]) * (1.0 / D) + EPS)
    query = jax.nn.silu(sum_a[0:8] * scale)
    query = query * lax.rsqrt(jnp.sum(query * query, axis=1, keepdims=True) + EPS) * (128 ** -0.5)
    keyed = jax.nn.silu(sum_a[8:16] * scale)
    keyed = keyed * lax.rsqrt(jnp.sum(keyed * keyed, axis=1, keepdims=True) + EPS)
    beta = jax.nn.sigmoid(extra[:, 0:1] * scale)
    rate = jnp.where(iota((8, 1), 0) < 4, ratev[0:1, 0:1], ratev[0:1, 1:2])
    decay = jnp.exp(-rate * jax.nn.softplus(extra[:, 1:2] * scale))
    key_t = jnp.transpose(keyed)
    query_t = jnp.transpose(query)
    recs = []
    for b in range(8):
        h, i = b // 4, b % 4
        recs.append(jnp.sum(st[i, h] * key_t[:, b:b + 1], axis=0, keepdims=True))
    recalled = jnp.concatenate(recs, axis=0)
    z_take(g_b, rb)
    sum_b = jnp.sum(rb[...].astype(F32), axis=0)
    valued = jax.nn.silu(sum_b[0:8] * scale)
    gate = jax.nn.silu(sum_b[8:16] * scale)
    write = beta * (valued - decay * recalled)
    reads = []
    for b in range(8):
        h, i = b // 4, b % 4
        fresh = decay[b:b + 1, :] * st[i, h] + key_t[:, b:b + 1] * write[b:b + 1, :]
        new_ref[i, h] = fresh
        reads.append(jnp.sum(fresh * query_t[:, b:b + 1], axis=0, keepdims=True))
    read = jnp.concatenate(reads, axis=0)
    mixed = read * lax.rsqrt(jnp.mean(read * read, axis=1, keepdims=True) + EPS) * hgainv[...] * gate
    mx[pl.ds(z, 1)] = mixed.astype(BF16)[None]
    z_gather(g_m, mx)

    def far_halves(group, buf):
        for from_y, at_row, to in ((yp(-1), 0, yp(1)), (yp(1), 32, yp(-1))):
            piece = buf.at[from_y, pl.ds(at_row, 32)]
            group.send(piece, piece, kv_of(z, to), tp)

    g_wu.take(wuf.at[pl.ds(0, 2)])
    far_halves(g_wu2, wuf)
    for d in (1, 3):
        y_send(g_wd, wdf, d)
    g_wo.take(wof.at[pl.ds(0, 3)])
    g_mg.take(mg.at[pl.ds(0, 3)])
    wov = wof[...].reshape(256, 256)
    z_take(g_m, mx)
    m = mx[...].astype(F32).reshape(128, 128).astype(BF16)
    mixed2 = jnp.concatenate([mm(heads_in[h], m) for h in range(2)], axis=1).astype(BF16)
    at[pl.ds(tp, 1)] = mm(mixed2, wov, NT_DIMS).astype(BF16)[None]
    g_t = wire.group("g_t")
    for d in (4, 5, 2, 3, 6, 7, 1):
        g_t.send(at.at[tp], at.at[tp], kv, tq(d))
    gain_mid = jnp.concatenate([mg[yy][0:1] for yy in range(NY)], axis=1)
    rr3, cc3 = iota((128, 64), 0), iota((128, 64), 1)
    row3 = 4 * (2 * ((rr3 % 64) // 8) + rr3 // 64) + rr3 % 4
    spread = [one_hot((cc3 == row3) & ((rr3 % 8) // 4 == c)) for c in range(2)]
    g_wu2.take(wuf.at[0])
    g_t.take(at.at[pl.ds(0, NT - 1)])
    attended = jnp.sum(at[...].astype(F32), axis=0)
    residual = (tok_rows + attended).astype(BF16)
    r32 = residual.astype(F32)
    gained_mid = (r32 * gain_mid).astype(BF16)
    lg = [mm(spread[c], gained_mid).astype(BF16) for c in range(2)]
    wu = wuf[...].reshape(256, 2048)
    g_u1, g_u2 = wire.group("g_u1"), wire.group("g_u2")
    par, m_here = z % 2, z // 2
    partner = (kv_of((z + 1 - 2 * par + NZ) % NZ, y), kv_of((z - 1 + 2 * par + NZ) % NZ, y))
    for f in range(2):
        lo, hi = 512 * f, 512 * (f + 1)
        up = mm(lg[0], wu[:, lo:hi]) + mm(lg[1], wu[:, 1024 + lo:1024 + hi])
        us[f] = up.reshape(2, 8, 8, 512).astype(BF16)
        g_u1.send(us.at[f, 1 - par], near.at[f], partner[f], tp)

    sq = r32 * r32
    sq_hi = sq.astype(BF16)
    sq_lo = (sq - sq_hi.astype(F32)).astype(BF16)
    ones = jnp.ones((8, 256), BF16)
    em[pl.ds(z, 1)] = (mm(ones, sq_hi, NT_DIMS) + mm(ones, sq_lo, NT_DIMS))[0:1][None]
    eye256 = one_hot(iota((256, 256), 0) == iota((256, 256), 1))

    def by_y(x):
        x = x.reshape(NY, 2, 32, 64)
        return jnp.concatenate([x[:, 0], x[:, 1]], axis=-1).astype(BF16)

    res_s[...] = by_y(mm(eye256, residual, NT_DIMS))
    res[pl.ds(y, 1)] = res_s[pl.ds(y, 1)]
    g_u1.take(near)
    def same_parity(e):
        return (m_here + e) % 8

    for f in range(2):
        pair = us[f, pl.ds(par, 1)][0].astype(F32) + near[f].astype(F32)
        fs[:, f] = pair.astype(BF16)
    for e in (4, 3, 5, 2, 6, 1, 7):
        g_u2.send(fs.at[same_parity(e)], ru.at[m_here], kv_of(2 * same_parity(e) + par, y), tp)
    ru[pl.ds(m_here, 1)] = fs[pl.ds(m_here, 1)]
    g_em, g_res = wire.group("g_em"), wire.group("g_res")
    z_gather(g_em, em)
    for d in (1, 3, 2):
        g_res.send(res_s.at[yp(d)], res.at[y], kv_of(z, yp(d)), tp)
    g_wd.take(wdf.at[pl.ds(0, 2)])
    far_halves(g_wd2, wdf)
    rr4, cc4 = iota((512, 256), 0), iota((512, 256), 1)
    row4 = 16 * ((rr4 % 64) // 4) + 4 * (rr4 // 128) + rr4 % 4
    for e in range(2):
        place[e] = one_hot((cc4 == row4) & ((rr4 % 128) // 64 == e))
    g_u2.take(ru.at[pl.ds(0, 7)])
    total = jnp.sum(ru[...].astype(F32), axis=0)
    hidden = jnp.square(jnp.maximum(total, 0.0)).astype(BF16)
    for f in range(2):
        hid[f, pl.ds(par, 1), pl.ds(m_here, 1)] = hidden[f][None, None]
    g_h1 = [wire.group("g_h1") for _ in range(7)]
    g_h2 = [wire.group("g_h2") for _ in range(2)]
    order = (4, 3, 5, 2, 6, 1, 7)
    for g, e in zip(g_h1, order):
        mine = hid.at[:, par, m_here]
        g.send(mine, mine, kv_of(2 * same_parity(e) + par, y), tp)

    def to_partners(slot):
        for f in range(2):
            piece = hid.at[f, par, slot]
            g_h2[f].send(piece, piece, partner[f], tp)

    to_partners(m_here)
    for g, e in zip(g_h1, order):
        g.take(hid.at[:, par, same_parity(8 - e)])
        to_partners(same_parity(8 - e))
    g_wd2.take(wdf.at[0])
    g_res.take(res.at[pl.ds(0, 3)])
    z_take(g_em, em)
    energy_mid = jnp.sum(em[...], axis=0)
    scale_mid = lax.rsqrt(energy_mid * (1.0 / D) + EPS)
    wd = wdf[...].reshape(256, 2048)
    for f in range(2):
        g_h2[f].take(hid.at[f, 1 - par])
    down = None
    for f in range(2):
        hv = hid[f].astype(F32).reshape(128, 512).astype(BF16)
        for c in range(2):
            rows = mm(hid_in[c], hv).astype(BF16)
            at_col = 1024 * c + 512 * f
            term = mm(wd[:, at_col:at_col + 512], rows, NT_DIMS)
            down = term if down is None else down + term
    fin_s[...] = by_y(down * (scale_mid * scale_mid))
    g_f = wire.group("g_f")
    for e in (2, 1, 3, 0):
        for d in (4, 5, 2, 3, 6, 7, 1, 0):
            if e == 0 and d == 0:
                continue
            g_f.send(fin_s.at[yp(e)], fin.at[tp * NY + y], kv_of(z, yp(e)), tq(d))
    fin[pl.ds(tp * NY + y, 1)] = fin_s[pl.ds(y, 1)]
    g_f.take(fin.at[pl.ds(0, 31)])
    mixer = jnp.sum(fin[...].astype(F32).reshape(NT, NY, 32, 128), axis=0)
    last = (res[...].astype(F32) + mixer).astype(BF16)
    flat = jnp.concatenate([last[yy] for yy in range(NY)], axis=1)
    for e in range(2):
        out_ref[pl.ds(32 * e, 32), :] = mm(flat, place[e]).astype(BF16)
    with jax.named_scope("finish"):
        wire.finish()


def body(
    tokens, mix_gain, w_query, w_key, w_value, w_gate, w_beta, w_decay, decay_rate, head_gain,
    state, w_out, mlp_gain, w_up, w_down,
):
    vmem = pl.BlockSpec(memory_space=pltpu.VMEM)
    hbm = pl.BlockSpec(memory_space=pltpu.HBM)
    v = pltpu.VMEM
    n_sem = 38
    out, new = pl.pallas_call(
        kernel,
        name="layer",
        out_shape=(
            pltpu.VMEM((64, 256), BF16),
            pltpu.VMEM((4, 2, 128, 128), F32),
        ),
        in_specs=[hbm] * 15,
        out_specs=(vmem, vmem),
        scratch_shapes=[
            v((64, 256), BF16), v((1, 64), F32), v((2, 64), BF16), v((2, 64), BF16),
            v((1, 2), F32), v((1, 128), F32), v((1, 64), F32),
            v((4, 64, 256), BF16), v((4, 64, 256), BF16), v((4, 64, 256), BF16), v((4, 64, 256), BF16),
            v((4, 64, 256), BF16), v((4, 64, 2048), BF16), v((4, 64, 2048), BF16),
            v((4, 2, 128, 128), F32),
            v((4, 64, 128), BF16), v((4, 64, 128), BF16), v((4, 8, 64), BF16), v((4, 8, 64), F32),
            v((16, 24, 128), BF16), v((16, 16, 128), BF16), v((16, 24, 128), BF16), v((16, 16, 128), BF16),
            v((16, 8, 128), BF16), v((8, 64, 256), BF16),
            v((2, 2, 8, 8, 512), BF16), v((2, 8, 8, 512), BF16), v((8, 2, 8, 512), BF16), v((8, 2, 8, 512), BF16),
            v((2, 2, 8, 8, 512), BF16), v((16, 1, 64), F32),
            v((4, 32, 128), BF16), v((4, 32, 128), BF16),
            v((4, 32, 128), BF16), v((32, 32, 128), BF16),
            v((2, 64, 128), BF16), v((2, 64, 128), BF16), v((2, 512, 256), BF16),
            pltpu.SemaphoreType.DMA((n_sem,)), pltpu.SemaphoreType.DMA((n_sem,)),
            pltpu.SemaphoreType.DMA((15,)),
        ],
        compiler_params=pltpu.CompilerParams(
            collective_id=0, has_side_effects=True, vmem_limit_bytes=66000000,
        ),
    )(
        tokens.T, mix_gain.reshape(1, 64), w_query, w_key, w_value, w_gate,
        w_beta.T, w_decay.T, decay_rate.reshape(1, 2), head_gain.reshape(1, 128), state, w_out.T,
        mlp_gain.reshape(1, 64), w_up, w_down.T,
    )
    return out.T, new


def solution(mesh):
    return jax.shard_map(
        body,
        mesh=mesh,
        in_specs=(
            P(None, "kv"), P("kv"), P("kv", "tp"), P("kv", "tp"), P("kv", "tp"), P("kv", "tp"),
            P("kv", "tp"), P("kv", "tp"), P("tp"), P(), P("kv", "tp", None, None),
            P("tp", "kv"), P("kv"), P("kv", "tp"), P("tp", "kv"),
        ),
        out_specs=(P(None, "kv"), P("kv", "tp", None, None)),
        check_vma=False,
    )
```

```python
import functools

import jax
import jax.numpy as jnp
from jax import lax
from jax.experimental import pallas as pl
from jax.experimental.pallas import tpu as pltpu
from jax.sharding import PartitionSpec as P

D = 4096
EPS = 1e-06
MESH = pl.DeviceIdType.MESH
F32 = jnp.float32
BF16 = jnp.bfloat16
NZ, NY, NT = 16, 4, 8
FAR_FIRST = (8, 7, 9, 6, 10, 5, 11, 4, 12, 3, 13, 2, 14, 1, 15)

NN = (((1,), (0,)), ((), ()))
NT_DIMS = (((1,), (1,)), ((), ()))


def mm(a, b, dims=NN):
    return lax.dot_general(a, b, dims, preferred_element_type=F32)


def iota(shape, dim):
    return lax.broadcasted_iota(jnp.int32, shape, dim)


def one_hot(cond):
    return jnp.where(cond, 1.0, 0.0).astype(BF16)


class Group:
    def __init__(self, wire, index, name):
        self.wire, self.index, self.name, self.total = wire, index, name, None

    def copy(self, src, dst, kv, tp):
        return pltpu.make_async_remote_copy(
            src, dst, self.wire.send_sem.at[self.index], self.wire.recv_sem.at[self.index],
            device_id={"kv": kv, "tp": tp}, device_id_type=MESH,
        )

    def send(self, src, dst, kv, tp):
        self.copy(src, dst, kv, tp).start()

    def take(self, total):
        self.total = total
        with jax.named_scope(self.name):
            self.copy(total, total, self.wire.kv, self.wire.tp).wait_recv()

    def finish(self):
        self.copy(self.total, self.total, self.wire.kv, self.wire.tp).wait_send()


class Wire:
    def __init__(self, send_sem, recv_sem, kv, tp):
        self.send_sem, self.recv_sem, self.kv, self.tp = send_sem, recv_sem, kv, tp
        self.groups = []

    def group(self, name):
        self.groups.append(Group(self, len(self.groups), name))
        return self.groups[-1]

    def finish(self):
        for group in self.groups:
            group.finish()


def kernel(
    tok_ref, mixg_ref, wq_ref, wk_ref, wv_ref, wg_ref, wb_ref, wdec_ref, rate_ref, hgain_ref,
    state_ref, wo_ref, mlpg_ref, wu_ref, wd_ref,
    out_ref, new_ref,
    tokv, mixv, wbv, wdecv, ratev, hgainv, mlpv,
    wqf, wkf, wvf, wgf, wof, wuf, wdf, st,
    tg_s, tg, sm, mg, sa, sb, ra, rb, mx, at, us, near, fs, ru, hid, em, res_s, res, fin_s, fin,
    heads_in, hid_in, place, send_sem, recv_sem, local_sem, known,
):
    kv, tp = lax.axis_index("kv"), lax.axis_index("tp")
    z, y = kv // NY, kv % NY

    def kv_of(zz, yy):
        return zz * NY + yy

    def zp(d):
        return (z + d) % NZ

    def yp(d):
        return (y + d) % NY

    def tq(d):
        return (tp + d) % NT

    def notify(sem, kv_t, tp_t):
        pl.semaphore_signal(sem, 1, device_id={"kv": kv_t, "tp": tp_t}, device_id_type=MESH)

    def partner_core():
        return tp + 1 - 2 * (tp % 2)

    barrier = pltpu.get_barrier_semaphore()
    for d in (1, NZ - 1):
        notify(barrier, kv_of(zp(d), y), tp)
    for d in (2, 1, 3):
        notify(barrier, kv_of(z, yp(d)), tp)
    for d in (4, 2, 6):
        notify(barrier, kv, tq(d))
    notify(barrier, kv, partner_core())

    loads = []
    for i, (src, dst) in enumerate((
        (tok_ref, tokv), (mixg_ref, mixv), (wb_ref, wbv), (wdec_ref, wdecv), (mlpg_ref, mlpv),
        (rate_ref, ratev), (hgain_ref, hgainv),
        (wq_ref, wqf.at[y]), (wk_ref, wkf.at[y]), (wv_ref, wvf.at[y]), (wg_ref, wgf.at[y]),
        (wo_ref, wof.at[y]), (wu_ref, wuf.at[y]), (wd_ref, wdf.at[y]), (state_ref, st),
    )):
        load = pltpu.make_async_copy(src, dst, local_sem.at[i])
        load.start()
        loads.append(load)

    with jax.named_scope("small_loads"):
        for i in range(7):
            loads[i].wait()

    r64, c64 = iota((64, 64), 0), iota((64, 64), 1)
    eye64 = one_hot(r64 == c64)
    gain_col = jnp.sum(jnp.where(r64 == c64, jnp.broadcast_to(mixv[...], (64, 64)), 0.0), axis=1, keepdims=True)
    tokt = tokv[...]
    gnt = (tokt.astype(F32) * gain_col).astype(BF16)
    rr, cc = iota((256, 128), 0), iota((256, 128), 1)
    cl = cc % 64
    for yy in range(NY):
        row_of = 16 * (cl // 4) + 4 * yy + cl % 4
        hit = rr == row_of
        pick_t = one_hot(hit & (cc < 64))
        pick_g = one_hot(hit & (cc >= 64))
        tg_s[yy] = (mm(tokt, pick_t) + mm(gnt, pick_g)).astype(BF16)
    mg[pl.ds(y, 1)] = jnp.broadcast_to(mlpv[...], (8, 64))[None]
    wb32, wdec32 = wbv[...].astype(F32), wdecv[...].astype(F32)
    r8 = iota((8, 64), 0)
    sm_rows = jnp.zeros((8, 64), F32)
    for k, row in enumerate((wb32[0:1], wb32[1:2], wdec32[0:1], wdec32[1:2])):
        sm_rows = jnp.where(r8 == k, jnp.broadcast_to(row, (8, 64)), sm_rows)
    sm[pl.ds(y, 1)] = sm_rows.astype(BF16)[None]
    tg[pl.ds(y, 1)] = tg_s[pl.ds(y, 1)]

    rr, cc = iota((128, 128), 0), iota((128, 128), 1)
    src_row = 4 * (rr // 8) + rr % 4
    half = (rr % 8) // 4
    q_g = [one_hot((cc == 64 + src_row) & (half == h)) for h in range(2)]
    q_t = one_hot(cc == src_row)
    rr2, cc2 = iota((64, 128), 0), iota((64, 128), 1)
    pick_tok = one_hot(cc2 == rr2)
    z2 = rr2 // 4
    for h in range(2):
        heads_in[h] = one_hot(cc2 == 8 * z2 + 4 * h + rr2 % 4)
        hid_in[h] = one_hot(cc2 == 64 * (z2 % 2) + 8 * (z2 // 2) + 4 * h + rr2 % 4)

    wire = Wire(send_sem, recv_sem, kv, tp)
    with jax.named_scope("barrier"):
        pl.semaphore_wait(barrier, 9)
    for d in (1, NZ - 1):
        notify(known.at[0], kv_of(zp(d), y), tp)
    for d in range(1, NY):
        notify(known.at[1], kv_of(z, yp(d)), tp)

    def y_send(group, buf, d, src=None):
        group.send(buf.at[y] if src is None else src, buf.at[y], kv_of(z, yp(d)), tp)

    g_tg, g_sm, g_mg = wire.group("g_tg"), wire.group("g_sm"), wire.group("g_mg")
    for d in (1, 3, 2):
        y_send(g_tg, tg, d, tg_s.at[yp(d)])
        y_send(g_sm, sm, d)
    for i in range(4):
        loads[7 + i].wait()
    full = (wqf, wkf, wvf, wgf)
    right = [wire.group("right") for _ in range(4)]
    left = [wire.group("left") for _ in range(4)]
    relay = [wire.group("relay") for _ in range(4)]
    for i in range(4):
        y_send(right[i], full[i], 1)
        y_send(left[i], full[i], 3)
    with jax.named_scope("known0"):
        pl.semaphore_wait(known.at[0], 2)
    for d in (2, NZ - 2):
        notify(known.at[2], kv_of(zp(d), y), tp)
    with jax.named_scope("known1"):
        pl.semaphore_wait(known.at[1], NY - 1)
    notify(known.at[3], kv, partner_core())

    def pass_on(a, b):
        right[a].take(full[a].at[yp(-1)])
        relay[a].send(full[a].at[yp(-1)], full[a].at[yp(-1)], kv_of(z, yp(1)), tp)
        left[b].take(full[b].at[yp(1)])
        relay[b].send(full[b].at[yp(1)], full[b].at[yp(1)], kv_of(z, yp(-1)), tp)

    g_tg.take(tg.at[pl.ds(0, 3)])
    g_sm.take(sm.at[pl.ds(0, 3)])
    with jax.named_scope("known2"):
        pl.semaphore_wait(known.at[2], 2)
    for d in (4, NZ - 4):
        notify(known.at[4], kv_of(zp(d), y), tp)
    pass_on(0, 1)
    tgv = tg[...].reshape(256, 128)
    lq = [mm(q_g[h], tgv, NT_DIMS).astype(BF16) for h in range(2)]
    tok_rows = mm(pick_tok, tgv, NT_DIMS)

    t32 = tgv.astype(F32)
    energy = jnp.sum(t32 * t32, axis=0, keepdims=True)
    e_hi = energy.astype(BF16)
    e_lo = (energy - e_hi.astype(F32)).astype(BF16)
    e_rows = jnp.where(rr == 2, jnp.broadcast_to(e_hi.astype(F32), (128, 128)),
                       jnp.where(rr == 3, jnp.broadcast_to(e_lo.astype(F32), (128, 128)), 0.0)).astype(BF16)
    small_out = mm(q_t, e_rows, NT_DIMS)
    for h in range(2):
        sel = one_hot(((iota((128, 8), 0) == 0) & (iota((128, 8), 1) == h))
                      | ((iota((128, 8), 0) == 1) & (iota((128, 8), 1) == 2 + h)))
        parts = [mm(eye64, mm(sel, sm[yy]).astype(BF16), NT_DIMS) for yy in range(NY)]
        w_small = jnp.concatenate(parts, axis=0).astype(BF16)
        small_out += mm(lq[h], w_small)
    pass_on(2, 3)
    with jax.named_scope("known3"):
        pl.semaphore_wait(known.at[3], 1)
        pl.semaphore_wait(known.at[4], 2)
    for i in range(11, 14):
        loads[i].wait()
    g_wo, g_wu, g_wu2 = wire.group("g_wo"), wire.group("g_wu"), wire.group("g_wu2")
    g_wd, g_wd2 = wire.group("g_wd"), wire.group("g_wd2")
    for d in (1, 3, 2):
        y_send(g_wo, wof, d)
    for d in (1, 3, 2):
        y_send(g_mg, mg, d)
    for d in (1, 3):
        y_send(g_wu, wuf, d)

    def project(buf):
        w = buf[...].reshape(256, 256)
        return mm(lq[0], w[:, :128]) + mm(lq[1], w[:, 128:])

    def stage(blocks):
        return jnp.concatenate([b.reshape(NZ, 8, 128) for b in blocks], axis=1).astype(BF16)

    def z_scatter(group, src, dst):
        for d in FAR_FIRST:
            group.send(src.at[zp(d)], dst.at[z], kv_of(zp(d), y), tp)

    def z_gather(group, buf):
        for d in FAR_FIRST:
            group.send(buf.at[z], buf.at[z], kv_of(zp(d), y), tp)

    def z_take(group, buf):
        group.take(buf.at[pl.ds(0, NZ - 1)])

    g_a, g_b, g_m = wire.group("g_a"), wire.group("g_b"), wire.group("g_m")
    left[0].take(wqf.at[yp(1)])
    relay[0].take(wqf.at[yp(2)])
    right[1].take(wkf.at[yp(-1)])
    relay[1].take(wkf.at[yp(2)])
    sa[...] = stage([project(wqf), project(wkf), small_out])
    z_scatter(g_a, sa, ra)
    left[2].take(wvf.at[yp(1)])
    relay[2].take(wvf.at[yp(2)])
    right[3].take(wgf.at[yp(-1)])
    relay[3].take(wgf.at[yp(2)])
    sb[...] = stage([project(wvf), project(wgf)])
    z_scatter(g_b, sb, rb)
    ra[pl.ds(z, 1)] = sa[pl.ds(z, 1)]
    rb[pl.ds(z, 1)] = sb[pl.ds(z, 1)]
    loads[14].wait()
    z_take(g_a, ra)
    sum_a = jnp.sum(ra[...].astype(F32), axis=0)
    extra = sum_a[16:24]
    scale = lax.rsqrt((extra[:, 2:3] + extra[:, 3:4]) * (1.0 / D) + EPS)
    query = jax.nn.silu(sum_a[0:8] * scale)
    query = query * lax.rsqrt(jnp.sum(query * query, axis=1, keepdims=True) + EPS) * (128 ** -0.5)
    keyed = jax.nn.silu(sum_a[8:16] * scale)
    keyed = keyed * lax.rsqrt(jnp.sum(keyed * keyed, axis=1, keepdims=True) + EPS)
    beta = jax.nn.sigmoid(extra[:, 0:1] * scale)
    rate = jnp.where(iota((8, 1), 0) < 4, ratev[0:1, 0:1], ratev[0:1, 1:2])
    decay = jnp.exp(-rate * jax.nn.softplus(extra[:, 1:2] * scale))
    key_t = jnp.transpose(keyed)
    query_t = jnp.transpose(query)
    recs = []
    for b in range(8):
        h, i = b // 4, b % 4
        recs.append(jnp.sum(st[i, h] * key_t[:, b:b + 1], axis=0, keepdims=True))
    recalled = jnp.concatenate(recs, axis=0)
    z_take(g_b, rb)
    sum_b = jnp.sum(rb[...].astype(F32), axis=0)
    valued = jax.nn.silu(sum_b[0:8] * scale)
    gate = jax.nn.silu(sum_b[8:16] * scale)
    write = beta * (valued - decay * recalled)
    reads = []
    for b in range(8):
        h, i = b // 4, b % 4
        fresh = decay[b:b + 1, :] * st[i, h] + key_t[:, b:b + 1] * write[b:b + 1, :]
        new_ref[i, h] = fresh
        reads.append(jnp.sum(fresh * query_t[:, b:b + 1], axis=0, keepdims=True))
    read = jnp.concatenate(reads, axis=0)
    mixed = read * lax.rsqrt(jnp.mean(read * read, axis=1, keepdims=True) + EPS) * hgainv[...] * gate
    mx[pl.ds(z, 1)] = mixed.astype(BF16)[None]
    z_gather(g_m, mx)

    def far_halves(group, buf):
        for from_y, at_row, to in ((yp(-1), 0, yp(1)), (yp(1), 32, yp(-1))):
            piece = buf.at[from_y, pl.ds(at_row, 32)]
            group.send(piece, piece, kv_of(z, to), tp)

    g_wu.take(wuf.at[pl.ds(0, 2)])
    far_halves(g_wu2, wuf)
    for d in (1, 3):
        y_send(g_wd, wdf, d)
    g_wo.take(wof.at[pl.ds(0, 3)])
    g_mg.take(mg.at[pl.ds(0, 3)])
    wov = wof[...].reshape(256, 256)
    z_take(g_m, mx)
    m = mx[...].astype(F32).reshape(128, 128).astype(BF16)
    mixed2 = jnp.concatenate([mm(heads_in[h], m) for h in range(2)], axis=1).astype(BF16)
    at[pl.ds(tp, 1)] = mm(mixed2, wov, NT_DIMS).astype(BF16)[None]
    g_t = wire.group("g_t")
    for d in (4, 5, 2, 3, 6, 7, 1):
        g_t.send(at.at[tp], at.at[tp], kv, tq(d))
    gain_mid = jnp.concatenate([mg[yy][0:1] for yy in range(NY)], axis=1)
    rr3, cc3 = iota((128, 64), 0), iota((128, 64), 1)
    row3 = 4 * (2 * ((rr3 % 64) // 8) + rr3 // 64) + rr3 % 4
    spread = [one_hot((cc3 == row3) & ((rr3 % 8) // 4 == c)) for c in range(2)]
    g_wu2.take(wuf.at[0])
    g_t.take(at.at[pl.ds(0, NT - 1)])
    attended = jnp.sum(at[...].astype(F32), axis=0)
    residual = (tok_rows + attended).astype(BF16)
    r32 = residual.astype(F32)
    gained_mid = (r32 * gain_mid).astype(BF16)
    lg = [mm(spread[c], gained_mid).astype(BF16) for c in range(2)]
    wu = wuf[...].reshape(256, 2048)
    g_u1, g_u2 = wire.group("g_u1"), wire.group("g_u2")
    par, m_here = z % 2, z // 2
    partner = (kv_of((z + 1 - 2 * par + NZ) % NZ, y), kv_of((z - 1 + 2 * par + NZ) % NZ, y))
    for f in range(2):
        lo, hi = 512 * f, 512 * (f + 1)
        up = mm(lg[0], wu[:, lo:hi]) + mm(lg[1], wu[:, 1024 + lo:1024 + hi])
        us[f] = up.reshape(2, 8, 8, 512).astype(BF16)
        g_u1.send(us.at[f, 1 - par], near.at[f], partner[f], tp)

    sq = r32 * r32
    sq_hi = sq.astype(BF16)
    sq_lo = (sq - sq_hi.astype(F32)).astype(BF16)
    ones = jnp.ones((8, 256), BF16)
    em[pl.ds(z, 1)] = (mm(ones, sq_hi, NT_DIMS) + mm(ones, sq_lo, NT_DIMS))[0:1][None]
    eye256 = one_hot(iota((256, 256), 0) == iota((256, 256), 1))

    def by_y(x):
        x = x.reshape(NY, 2, 32, 64)
        return jnp.concatenate([x[:, 0], x[:, 1]], axis=-1).astype(BF16)

    res_s[...] = by_y(mm(eye256, residual, NT_DIMS))
    res[pl.ds(y, 1)] = res_s[pl.ds(y, 1)]
    g_u1.take(near)
    def same_parity(e):
        return (m_here + e) % 8

    for f in range(2):
        pair = us[f, pl.ds(par, 1)][0].astype(F32) + near[f].astype(F32)
        fs[:, f] = pair.astype(BF16)
    for e in (4, 3, 5, 2, 6, 1, 7):
        g_u2.send(fs.at[same_parity(e)], ru.at[m_here], kv_of(2 * same_parity(e) + par, y), tp)
    ru[pl.ds(m_here, 1)] = fs[pl.ds(m_here, 1)]
    g_em, g_res = wire.group("g_em"), wire.group("g_res")
    z_gather(g_em, em)
    for d in (1, 3, 2):
        g_res.send(res_s.at[yp(d)], res.at[y], kv_of(z, yp(d)), tp)
    g_wd.take(wdf.at[pl.ds(0, 2)])
    far_halves(g_wd2, wdf)
    rr4, cc4 = iota((512, 256), 0), iota((512, 256), 1)
    row4 = 16 * ((rr4 % 64) // 4) + 4 * (rr4 // 128) + rr4 % 4
    for e in range(2):
        place[e] = one_hot((cc4 == row4) & ((rr4 % 128) // 64 == e))
    g_u2.take(ru.at[pl.ds(0, 7)])
    total = jnp.sum(ru[...].astype(F32), axis=0)
    hidden = jnp.square(jnp.maximum(total, 0.0)).astype(BF16)
    for f in range(2):
        hid[f, pl.ds(par, 1), pl.ds(m_here, 1)] = hidden[f][None, None]
    g_h1 = [wire.group("g_h1") for _ in range(7)]
    g_h2 = [wire.group("g_h2") for _ in range(2)]
    order = (4, 3, 5, 2, 6, 1, 7)
    for g, e in zip(g_h1, order):
        mine = hid.at[:, par, m_here]
        g.send(mine, mine, kv_of(2 * same_parity(e) + par, y), tp)

    def to_partners(slot):
        for f in range(2):
            piece = hid.at[f, par, slot]
            g_h2[f].send(piece, piece, partner[f], tp)

    to_partners(m_here)
    for g, e in zip(g_h1, order):
        g.take(hid.at[:, par, same_parity(8 - e)])
        to_partners(same_parity(8 - e))
    g_wd2.take(wdf.at[0])
    g_res.take(res.at[pl.ds(0, 3)])
    z_take(g_em, em)
    energy_mid = jnp.sum(em[...], axis=0)
    scale_mid = lax.rsqrt(energy_mid * (1.0 / D) + EPS)
    wd = wdf[...].reshape(256, 2048)
    for f in range(2):
        g_h2[f].take(hid.at[f, 1 - par])
    down = None
    for f in range(2):
        hv = hid[f].astype(F32).reshape(128, 512).astype(BF16)
        for c in range(2):
            rows = mm(hid_in[c], hv).astype(BF16)
            at_col = 1024 * c + 512 * f
            term = mm(wd[:, at_col:at_col + 512], rows, NT_DIMS)
            down = term if down is None else down + term
    fin_s[...] = by_y(down * (scale_mid * scale_mid))
    g_f = wire.group("g_f")
    for e in (2, 1, 3, 0):
        for d in (4, 5, 2, 3, 6, 7, 1, 0):
            if e == 0 and d == 0:
                continue
            g_f.send(fin_s.at[yp(e)], fin.at[tp * NY + y], kv_of(z, yp(e)), tq(d))
    fin[pl.ds(tp * NY + y, 1)] = fin_s[pl.ds(y, 1)]
    g_f.take(fin.at[pl.ds(0, 31)])
    mixer = jnp.sum(fin[...].astype(F32).reshape(NT, NY, 32, 128), axis=0)
    last = (res[...].astype(F32) + mixer).astype(BF16)
    flat = jnp.concatenate([last[yy] for yy in range(NY)], axis=1)
    for e in range(2):
        out_ref[pl.ds(32 * e, 32), :] = mm(flat, place[e]).astype(BF16)
    with jax.named_scope("finish"):
        wire.finish()


def body(
    tokens, mix_gain, w_query, w_key, w_value, w_gate, w_beta, w_decay, decay_rate, head_gain,
    state, w_out, mlp_gain, w_up, w_down,
):
    vmem = pl.BlockSpec(memory_space=pltpu.VMEM)
    hbm = pl.BlockSpec(memory_space=pltpu.HBM)
    v = pltpu.VMEM
    n_sem = 38
    out, new = pl.pallas_call(
        kernel,
        name="layer",
        out_shape=(
            pltpu.VMEM((64, 256), BF16),
            pltpu.VMEM((4, 2, 128, 128), F32),
        ),
        in_specs=[hbm] * 15,
        out_specs=(vmem, vmem),
        scratch_shapes=[
            v((64, 256), BF16), v((1, 64), F32), v((2, 64), BF16), v((2, 64), BF16),
            v((1, 2), F32), v((1, 128), F32), v((1, 64), F32),
            v((4, 64, 256), BF16), v((4, 64, 256), BF16), v((4, 64, 256), BF16), v((4, 64, 256), BF16),
            v((4, 64, 256), BF16), v((4, 64, 2048), BF16), v((4, 64, 2048), BF16),
            v((4, 2, 128, 128), F32),
            v((4, 64, 128), BF16), v((4, 64, 128), BF16), v((4, 8, 64), BF16), v((4, 8, 64), F32),
            v((16, 24, 128), BF16), v((16, 16, 128), BF16), v((16, 24, 128), BF16), v((16, 16, 128), BF16),
            v((16, 8, 128), BF16), v((8, 64, 256), BF16),
            v((2, 2, 8, 8, 512), BF16), v((2, 8, 8, 512), BF16), v((8, 2, 8, 512), BF16), v((8, 2, 8, 512), BF16),
            v((2, 2, 8, 8, 512), BF16), v((16, 1, 64), F32),
            v((4, 32, 128), BF16), v((4, 32, 128), BF16),
            v((4, 32, 128), BF16), v((32, 32, 128), BF16),
            v((2, 64, 128), BF16), v((2, 64, 128), BF16), v((2, 512, 256), BF16),
            pltpu.SemaphoreType.DMA((n_sem,)), pltpu.SemaphoreType.DMA((n_sem,)),
            pltpu.SemaphoreType.DMA((15,)), pltpu.SemaphoreType.REGULAR((5,)),
        ],
        compiler_params=pltpu.CompilerParams(
            collective_id=0, has_side_effects=True, vmem_limit_bytes=66000000,
        ),
    )(
        tokens.T, mix_gain.reshape(1, 64), w_query, w_key, w_value, w_gate,
        w_beta.T, w_decay.T, decay_rate.reshape(1, 2), head_gain.reshape(1, 128), state, w_out.T,
        mlp_gain.reshape(1, 64), w_up, w_down.T,
    )
    return out.T, new


def solution(mesh):
    return jax.shard_map(
        body,
        mesh=mesh,
        in_specs=(
            P(None, "kv"), P("kv"), P("kv", "tp"), P("kv", "tp"), P("kv", "tp"), P("kv", "tp"),
            P("kv", "tp"), P("kv", "tp"), P("tp"), P(), P("kv", "tp", None, None),
            P("tp", "kv"), P("kv"), P("kv", "tp"), P("tp", "kv"),
        ),
        out_specs=(P(None, "kv"), P("kv", "tp", None, None)),
        check_vma=False,
    )
```
